32 devices in a mesh: sp: 8 (over z, x), tp: 4 (over y, core).
Axes of the slice: x: 2, y: 2, z: 4, core: 2. Of those that a mesh axis runs over, the one named last changes fastest.
Arguments:
- mixer_input: bfloat16 [2048, 1024], P('sp', 'tp'), may hold values from -8 to 8
- decay_shift: float32 [2048, 64], P('sp', 'tp'), may hold values from -2.3 to 0
- pole_real: float32 [64, 64], P('tp'), may hold values from -1 to 0
- pole_imaginary: float32 [64, 64], P('tp'), may hold values from 1 to 201.06176
- log_step: float32 [64], P('tp'), may hold values from -4.15 to -3
- input_map: float32 [2, 64, 64, 16], P(None, 'tp'), may hold values from -1 to 1
- readout_matrix: float32 [2, 64, 16, 64], P(None, 'tp'), may hold values from -0.5 to 0.5
- skip: float32 [1024], P('tp'), may hold values from -6 to 6
- out_proj: bfloat16 [1024, 2048], P('tp'), may hold values from -0.1875 to 0.1875
- stream: bfloat16 [2048, 2048], P(('sp', 'tp')), may hold values from -6 to 6
- norm_gain: float32 [2048], replicated, may hold values from 0.1 to 1.9
- routes: int32 [2048, 2], P(('sp', 'tp')), may hold values from 0 to 7, all different within a row; in each aligned block of 64 rows (0 to 63, 64 to 127, ...) at most 32 rows name the same one
- route_logits: float32 [2048, 2], P(('sp', 'tp')), may hold values from -7.5 to 7.5
- w_gate: bfloat16 [8, 2048, 7168], P('sp', None, 'tp'), may hold values from -0.125 to 0.125
- w_up: bfloat16 [8, 2048, 7168], P('sp', None, 'tp'), may hold values from -0.125 to 0.125
- w_down: bfloat16 [8, 7168, 2048], P('sp', 'tp'), may hold values from -0.21875 to 0.21875
Outputs:
- layer_out: bfloat16 [2048, 2048], P(('sp', 'tp'))
The draws below stay inside these ranges and needn't reach their ends.
Inputs may be any that keep to these rules, and one draw needn't show every extreme that they name: `routes`: in the rows of one device no expert is named more than 32 times, a bound that some block reaches; the 2 experts of a token differ.
All inputs are finite; a program needn't handle non-finite values.
Results may differ from the reference program's by a relative error of at most 0.015.
Values may be sent and summed in bfloat16 or wider, within the bound.
A program may use at most 128 MiB of HBM per device.

```python
import math
import jax
import jax.numpy as jnp
import numpy as np
from jax import lax

D = 2048
GROUPS = 64
GROUP_CH = 16
STATE = 64
EXPERT_FF = 7168
TOP = 2
SEQUENCE_LOCAL = 256
MIXER_CHANNELS = 1024
SEQ = 2048
TOK_DEV = 64
EXPERTS = 8
CAP = 32
N_TP = 4


def quick_groups(key, count):
    order = jax.random.permutation(jax.random.fold_in(key, 101), GROUPS)
    return order < count


def step_logs(key, quick):
    keys = jax.random.split(jax.random.fold_in(key, 211), 2)
    fast = jax.random.uniform(keys[0], (GROUPS,), jnp.float32, -4.15, -3.88)
    slow = jax.random.uniform(keys[1], (GROUPS,), jnp.float32, -3.9, -3.0)
    return jnp.where(quick, fast, slow)


def draw_log_step(key, part):
    count = GROUPS // 2
    return step_logs(key, quick_groups(key, count))


def draw_pole_real(key, part):
    count = GROUPS // 2
    quick = quick_groups(key, count)
    keys = jax.random.split(jax.random.fold_in(key, 11), 2)
    quick_rate = jax.random.uniform(keys[0], (GROUPS, STATE), jnp.float32, 0.6, 1.0)
    slow_rate = jnp.exp(jax.random.uniform(keys[1], (GROUPS, STATE), jnp.float32, math.log(2.0 / SEQ), math.log(20.0 / SEQ)))
    return -jnp.where(quick[:, None], quick_rate, slow_rate)


def draw_pole_imaginary(key, part):
    count = GROUPS // 2
    quick = quick_groups(key, count)
    step = jnp.exp(step_logs(key, quick))
    keys = jax.random.split(jax.random.fold_in(key, 307), 3)
    spread_poles = jax.random.uniform(keys[0], (GROUPS, STATE), jnp.float32, 1.0, 3.14159 * STATE)
    jitter = jax.random.uniform(keys[1], (GROUPS, STATE), jnp.float32, -0.03, 0.03)
    adjusted = jnp.minimum((3.14159 + jitter) / step[:, None], 3.14159 * STATE)
    chosen = jax.random.randint(keys[2], (GROUPS, STATE), 0, 3) == 0
    return jnp.where(quick[:, None] & chosen, adjusted, spread_poles)


def draw_decay_shift(key, part):
    count = GROUPS // 2
    quick = quick_groups(key, count)
    keys = jax.random.split(jax.random.fold_in(key, 23), 5)
    blocks = SEQ // SEQUENCE_LOCAL
    level = jnp.exp(jax.random.uniform(keys[0], (blocks, GROUPS), jnp.float32, math.log(0.25), math.log(2.0)))
    pieces = jnp.exp(jax.random.uniform(keys[1], (SEQ // 32, GROUPS), jnp.float32, math.log(0.5), math.log(2.0)))
    rough = jax.random.uniform(keys[2], (SEQ, GROUPS), jnp.float32, 0.5, 1.5)
    rate = jnp.where(quick, 0.015, 0.8 / SEQ)
    steady = -jnp.repeat(level, SEQUENCE_LOCAL, axis=0) * jnp.repeat(pieces, 32, axis=0) * rough * rate[None, :]
    spots = jax.random.randint(keys[3], (3,), 0, SEQ)
    losses = jax.random.uniform(keys[4], (3, GROUPS), jnp.float32, math.log(0.5), math.log(0.8))
    hits = (jnp.arange(SEQ, dtype=jnp.int32)[:, None] == spots[None, :]).astype(jnp.float32)
    return steady + jnp.dot(hits, losses, precision=lax.Precision.HIGHEST)


def draw_mixer_input(key, part):
    keys = jax.random.split(jax.random.fold_in(key, 401), 2)
    noise = jnp.clip(jax.random.normal(keys[0], (SEQ, MIXER_CHANNELS), jnp.float32), -6.0, 6.0)
    amplitude = jax.random.uniform(keys[1], (MIXER_CHANNELS,), jnp.float32, -2.0, 2.0)
    parity = (1 - 2 * (jnp.arange(SEQ, dtype=jnp.int32) % 2)).astype(jnp.float32)
    return (noise + parity[:, None] * amplitude[None, :]).astype(jnp.bfloat16)


def draw_route_logits(key, part):
    keys = jax.random.split(jax.random.fold_in(key, 503), 3)
    leading = jnp.clip(1.5 * jax.random.normal(keys[0], (SEQ,), jnp.float32), -4.5, 4.5)
    spacing = jax.random.uniform(keys[1], (SEQ,), jnp.float32, 2.0, 3.0)
    direction = (2 * jax.random.randint(keys[2], (SEQ,), 0, 2) - 1).astype(jnp.float32)
    return jnp.stack([leading, leading - direction * spacing], axis=1)


def levels(key, dims, cuts, least, top_value):
    factor_of, own = 1.0, jax.random.fold_in(key, 6)
    for axis_at, parts in cuts:
        heights = jnp.exp(jax.random.uniform(jax.random.fold_in(own, axis_at), (parts,), jnp.float32, least / len(cuts), top_value / len(cuts)))
        factor_of = factor_of * jnp.repeat(heights, dims[axis_at] // parts).reshape([-1 if axis == axis_at else 1 for axis in range(len(dims))])
    return factor_of


def assign_block(rng, own, number, rows, amount, top, most, lean):
    sequence = jax.random.permutation(rng, amount)
    crowded, common = shares(amount, rows * top, most, lean, True), shares(amount, rows * top, most, lean, False)
    places = jnp.arange(amount)

    def named(sizes, offset_by):
        used = int((sizes > 0).sum())
        fixed = max(1, used // 4)
        moved = fixed + (places - fixed + offset_by * (used - fixed)) % max(1, amount - fixed)
        return jnp.zeros((amount,), jnp.int32).at[sequence[jnp.where(places < fixed, places, moved)]].set(jnp.asarray(sizes, jnp.int32))

    sizes = jnp.where(number % 4 == 0, named(crowded, number // 4), named(common, number - number // 4 - 1))
    mixed = jax.random.permutation(jax.random.fold_in(own, 3), amount)
    source_of, receiver = mixed[0:amount // 2 * 2:2], mixed[1:amount // 2 * 2:2]
    slack = jnp.minimum(sizes[source_of] - 1, most - sizes[receiver]) // 2
    slack = jnp.where((source_of == sequence[0]) | (receiver == sequence[0]) | (sizes[receiver] == 0), 0, jnp.maximum(slack, 0))
    moved = jax.random.randint(jax.random.fold_in(own, 4), (amount // 2,), 0, 1 << 20) % (slack + 1)
    sizes = sizes.at[source_of].add(-moved).at[receiver].add(moved)
    items = jnp.searchsorted(jnp.cumsum(sizes), jnp.arange(rows * top), side="right").astype(jnp.int32)
    table = items.reshape(top, rows).T
    table = table[jax.random.permutation(jax.random.fold_in(own, 1), rows)]
    offset_by = jax.random.randint(jax.random.fold_in(own, 2), (rows, 1), 0, top)
    return jnp.take_along_axis(table, (jnp.arange(top)[None, :] + offset_by) % top, axis=1)


def shares(number_of, total, reach, slope, full):
    weights = [(1 << 20) // math.isqrt(rank ** slope) + 1 for rank in range(1, number_of + 1)]
    largest = reach if full else min(reach, max(-(-total // number_of), total * weights[0] // sum(weights)))
    least = 1 if total - largest >= number_of - 1 else 0
    counts, rest = [largest] + [least] * (number_of - 1), total - largest - least * (number_of - 1)
    while rest > 0:
        free = [i for i in range(1, number_of) if counts[i] < largest] or [i for i in range(1, number_of) if counts[i] < reach]
        mass, remaining = sum([weights[i] for i in free]), rest
        for i in free:
            addition = min(reach - counts[i], max(1, remaining * weights[i] // mass), rest)
            counts[i] = counts[i] + addition
            rest = rest - addition
    return np.array(counts)


def gaussian(key, extent, spread, most, cuts=(), kind=jnp.bfloat16):
    factor_of = levels(key, extent, cuts, -0.22, 0.18) if cuts else 1.0
    entries = jax.random.normal(key, extent, jnp.float32) * spread * factor_of
    return jnp.minimum(jnp.maximum(entries, -most), most).astype(kind)


def setup_inputs(seed: int = 0) -> dict:
    key_list = jax.random.split(jax.random.key(seed), 17)
    mixer_input = draw_mixer_input(jax.random.fold_in(key_list[16], 71), 0)
    decay_shift = draw_decay_shift(jax.random.fold_in(key_list[16], 71), 0)
    pole_real = draw_pole_real(jax.random.fold_in(key_list[16], 71), 0)
    pole_imaginary = draw_pole_imaginary(jax.random.fold_in(key_list[16], 71), 0)
    log_step = draw_log_step(jax.random.fold_in(key_list[16], 71), 0)
    input_map = gaussian(key_list[5], (2, GROUPS, STATE, GROUP_CH), (2 * GROUP_CH) ** -0.5, 1.0, ((1, 4),), jnp.float32)
    readout_matrix = gaussian(key_list[6], (2, GROUPS, GROUP_CH, STATE), (2 * STATE) ** -0.5, 0.5, ((1, 4),), jnp.float32)
    skip = gaussian(key_list[7], (MIXER_CHANNELS,), 1.0, 6.0, ((0, 4),), jnp.float32)
    out_proj = gaussian(key_list[8], (MIXER_CHANNELS, D), MIXER_CHANNELS ** -0.5, 0.1875, ((0, 4),))
    stream = gaussian(key_list[9], (SEQ, D), 1.0, 6.0, ((0, 32),))
    norm_gain = jnp.clip(1.0 + 0.18 * jax.random.normal(key_list[10], (D,), jnp.float32), 0.1, 1.9)
    routes_keys = jax.random.split(jax.random.fold_in(key_list[11], 1), SEQ // TOK_DEV)
    routes_turns = jax.random.permutation(jax.random.fold_in(key_list[11], 3), SEQ // TOK_DEV)
    routes = jax.vmap(lambda own, number: assign_block(jax.random.fold_in(key_list[11], 2), own, number, TOK_DEV, EXPERTS, TOP, CAP, 2))(routes_keys, routes_turns).reshape((SEQ, TOP))
    route_logits = draw_route_logits(jax.random.fold_in(key_list[16], 71), 0)
    w_gate = gaussian(key_list[13], (EXPERTS, D, EXPERT_FF), D ** -0.5, 0.125, ((0, 8), (2, 4)))
    w_up = gaussian(key_list[14], (EXPERTS, D, EXPERT_FF), D ** -0.5, 0.125, ((0, 8), (2, 4)))
    w_down = gaussian(key_list[15], (EXPERTS, EXPERT_FF, D), (EXPERT_FF // 9) ** -0.5, 0.21875, ((0, 8), (1, 4)))
    return dict(mixer_input=mixer_input, decay_shift=decay_shift, pole_real=pole_real, pole_imaginary=pole_imaginary, log_step=log_step, input_map=input_map, readout_matrix=readout_matrix, skip=skip, out_proj=out_proj, stream=stream, norm_gain=norm_gain, routes=routes, route_logits=route_logits, w_gate=w_gate, w_up=w_up, w_down=w_down)


TOP_PRECISION = lax.Precision.HIGHEST
EPS = 1e-06
SEGMENT = 16

def discretize(pole_real, pole_imaginary, log_step, input_map):
    step = jnp.exp(log_step)[:, None]
    magnitude = jnp.exp(pole_real * step)
    factor_real = magnitude * jnp.cos(pole_imaginary * step)
    factor_imaginary = magnitude * jnp.sin(pole_imaginary * step)
    denominator = pole_real * pole_real + pole_imaginary * pole_imaginary
    ratio_real = ((factor_real - 1.0) * pole_real + factor_imaginary * pole_imaginary) / denominator
    ratio_imaginary = (factor_imaginary * pole_real - (factor_real - 1.0) * pole_imaginary) / denominator
    map_real = ratio_real[:, :, None] * input_map[0] - ratio_imaginary[:, :, None] * input_map[1]
    map_imaginary = ratio_real[:, :, None] * input_map[1] + ratio_imaginary[:, :, None] * input_map[0]
    return (factor_real, factor_imaginary, map_real, map_imaginary)

def link(earlier, later):
    a_real, a_imag_part, x_real, x_imag_part = earlier
    b_real, b_imag_part, y_real, y_imag_part = later
    return (b_real * a_real - b_imag_part * a_imag_part, b_real * a_imag_part + b_imag_part * a_real, b_real * x_real - b_imag_part * x_imag_part + y_real, b_real * x_imag_part + b_imag_part * x_real + y_imag_part)

def block_states(drive_input, shift, factors):
    factor_real, factor_imaginary, map_real, map_imaginary = factors
    rows, groups = shift.shape
    states = factor_real.shape[1]
    width = groups * states
    grouped = drive_input.reshape(rows, groups, -1)
    drive_real = jnp.einsum('sgc,gpc->sgp', grouped, map_real, precision=TOP_PRECISION).reshape(rows, width)
    drive_imaginary = jnp.einsum('sgc,gpc->sgp', grouped, map_imaginary, precision=TOP_PRECISION).reshape(rows, width)
    scale = jnp.exp(shift)[:, :, None]
    trans_real = (scale * factor_real[None]).reshape(rows, width)
    trans_imaginary = (scale * factor_imaginary[None]).reshape(rows, width)
    segments = rows // SEGMENT

    def arrange(value):
        return jnp.swapaxes(value.reshape(segments, SEGMENT, width), 0, 1)

    def advance(carry, item):
        new = link(carry, item)
        return (new, new)
    first = jnp.ones((segments, width), jnp.float32)
    empty = jnp.zeros((segments, width), jnp.float32)
    _, inner = lax.scan(advance, (first, empty, empty, empty), (arrange(trans_real), arrange(trans_imaginary), arrange(drive_real), arrange(drive_imaginary)))
    totals = tuple((part[-1] for part in inner))
    running = lax.associative_scan(link, totals, axis=0)
    enter = tuple((jnp.concatenate([start, part[:-1]], axis=0) for start, part in zip((first[:1], empty[:1], empty[:1], empty[:1]), running)))
    enter = tuple((part.reshape(segments, width) for part in enter))
    joined = link(tuple((part[None] for part in enter)), inner)

    def restore(value):
        return jnp.swapaxes(value, 0, 1).reshape(rows, groups, states)
    return tuple((restore(part) for part in joined))

def read_out(hidden_state_real, hidden_state_imaginary, readout_matrix):
    return jnp.einsum('ani,nyi->any', hidden_state_real, readout_matrix[0], precision=TOP_PRECISION) - jnp.einsum('ani,nyi->any', hidden_state_imaginary, readout_matrix[1], precision=TOP_PRECISION)

def reference(mixer_input, decay_shift, pole_real, pole_imaginary, log_step, input_map, readout_matrix, skip, out_proj, stream, norm_gain, routes, route_logits, w_gate, w_up, w_down):
    factors = discretize(pole_real, pole_imaginary, log_step, input_map)
    blocks = SEQ // SEQUENCE_LOCAL
    inputs_blocked = mixer_input.astype(jnp.float32).reshape(blocks, SEQUENCE_LOCAL, MIXER_CHANNELS)
    shift_blocked = decay_shift.reshape(blocks, SEQUENCE_LOCAL, GROUPS)

    def advance(carry, pair):
        drive_input, shift = pair
        through_real, through_imaginary, local_real, local_imaginary = block_states(drive_input, shift, factors)
        enter_real, enter_imaginary = carry
        hidden_state_real = local_real + through_real * enter_real[None] - through_imaginary * enter_imaginary[None]
        hidden_state_imaginary = local_imaginary + through_real * enter_imaginary[None] + through_imaginary * enter_real[None]
        response = read_out(hidden_state_real, hidden_state_imaginary, readout_matrix).reshape(SEQUENCE_LOCAL, MIXER_CHANNELS) + skip * drive_input
        activated = jax.nn.gelu(response).astype(jnp.bfloat16)
        return ((hidden_state_real[-1], hidden_state_imaginary[-1]), activated)
    start = (jnp.zeros((GROUPS, STATE), jnp.float32), jnp.zeros((GROUPS, STATE), jnp.float32))
    _, activated = lax.scan(advance, start, (inputs_blocked, shift_blocked))
    projected = jnp.dot(activated.reshape(SEQ, MIXER_CHANNELS), out_proj, preferred_element_type=jnp.float32)
    mixed = (stream.astype(jnp.float32) + projected).astype(jnp.bfloat16)
    mixed_wide = mixed.astype(jnp.float32)
    normed = (mixed_wide * lax.rsqrt(lax.optimization_barrier(jnp.mean(mixed_wide * mixed_wide, axis=-1, keepdims=True)) + EPS) * norm_gain).astype(jnp.bfloat16)
    device_blocks = SEQ // TOK_DEV
    assign = routes.reshape(device_blocks, TOK_DEV * TOP)
    matches = (assign[:, :, None] == jnp.arange(EXPERTS, dtype=jnp.int32)).astype(jnp.int32)
    rank = lax.optimization_barrier(jnp.sum((jnp.cumsum(matches, axis=1) - matches) * matches, axis=2))
    block_ids = jnp.broadcast_to(jnp.arange(device_blocks, dtype=jnp.int32)[:, None], assign.shape)
    token_ids = (jnp.arange(SEQ * TOP, dtype=jnp.int32) // TOP).reshape(device_blocks, TOK_DEV * TOP)
    buffer = jnp.zeros((EXPERTS, device_blocks, CAP, D), jnp.bfloat16)
    buffer = buffer.at[assign, block_ids, rank].set(normed[token_ids])

    def run_expert(pack):
        rows, gate_weight, upward_weight, down_weight = pack
        flat = rows.reshape(device_blocks * CAP, D)
        gate = jnp.dot(flat, gate_weight, preferred_element_type=jnp.float32)
        upward = jnp.dot(flat, upward_weight, preferred_element_type=jnp.float32)
        hidden = (jax.nn.silu(gate) * upward).astype(jnp.bfloat16)
        width = EXPERT_FF // N_TP
        summed = jnp.zeros((device_blocks * CAP, D), jnp.float32)
        for part_index in range(N_TP):
            partial_out = jnp.dot(hidden[:, part_index * width:(part_index + 1) * width], down_weight[part_index * width:(part_index + 1) * width], preferred_element_type=jnp.float32)
            summed = summed + lax.optimization_barrier(partial_out.astype(jnp.bfloat16)).astype(jnp.float32)
        return summed.astype(jnp.bfloat16).reshape(device_blocks, CAP, D)
    outputs = lax.map(run_expert, (buffer, w_gate, w_up, w_down))
    picked = outputs[assign, block_ids, rank].astype(jnp.float32).reshape(SEQ, TOP, D)
    logits = route_logits
    weights = jax.nn.sigmoid(jnp.stack([logits[:, 0] - logits[:, 1], logits[:, 1] - logits[:, 0]], axis=1))
    combined = mixed_wide + lax.optimization_barrier(jnp.sum(picked * weights[:, :, None], axis=1))
    return combined.astype(jnp.bfloat16)
```

```python
import functools

import jax
import jax.numpy as jnp
from jax import lax
from jax.experimental import pallas as pl
from jax.experimental.pallas import tpu as pltpu
from jax.sharding import PartitionSpec as P

TOP_PRECISION = lax.Precision.HIGHEST
EPS = 1e-06
LANES = 8
MESH = pl.DeviceIdType.MESH


def discretize(pole_real, pole_imaginary, log_step, input_map):
    step = jnp.exp(log_step)[:, None]
    magnitude = jnp.exp(pole_real * step)
    factor_real = magnitude * jnp.cos(pole_imaginary * step)
    factor_imaginary = magnitude * jnp.sin(pole_imaginary * step)
    denominator = pole_real * pole_real + pole_imaginary * pole_imaginary
    ratio_real = ((factor_real - 1.0) * pole_real + factor_imaginary * pole_imaginary) / denominator
    ratio_imaginary = (
        factor_imaginary * pole_real - (factor_real - 1.0) * pole_imaginary
    ) / denominator
    map_real = ratio_real[:, :, None] * input_map[0] - ratio_imaginary[:, :, None] * input_map[1]
    map_imaginary = (
        ratio_real[:, :, None] * input_map[1] + ratio_imaginary[:, :, None] * input_map[0]
    )
    return (factor_real, factor_imaginary, map_real, map_imaginary)


def on_ring(body, axis):
    count, mine = lax.axis_size(axis), lax.axis_index(axis)
    barrier = pltpu.get_barrier_semaphore()
    for ahead in range(1, count):
        pl.semaphore_signal(
            barrier,
            inc=1,
            device_id={axis: lax.rem(mine + ahead, count)},
            device_id_type=MESH,
        )
    pl.semaphore_wait(barrier, count - 1)
    body(count, mine)


def exchange_kernel(axis, gather, value, result, send, receive, own):
    def body(count, mine):
        copies = []
        for ahead in range(1, count):
            peer = lax.rem(mine + ahead, count)
            copy = pltpu.make_async_remote_copy(
                src_ref=value if gather else value.at[peer],
                dst_ref=result.at[mine],
                send_sem=send.at[ahead],
                recv_sem=receive.at[ahead],
                device_id={axis: peer},
                device_id_type=MESH,
            )
            copy.start()
            copies.append(copy)
        kept = pltpu.make_async_copy(value if gather else value.at[mine], result.at[mine], own)
        kept.start()
        kept.wait()
        for copy in copies:
            copy.wait()

    on_ring(body, axis)


def exchange(value, axis, number, gather=False):
    count = lax.axis_size(axis)
    shape = ((count,) + value.shape) if gather else value.shape
    return pl.pallas_call(
        functools.partial(exchange_kernel, axis, gather),
        out_shape=jax.ShapeDtypeStruct(shape, value.dtype),
        in_specs=[pl.BlockSpec(memory_space=pltpu.VMEM)],
        out_specs=pl.BlockSpec(memory_space=pltpu.VMEM),
        scratch_shapes=[
            pltpu.SemaphoreType.DMA((count,)),
            pltpu.SemaphoreType.DMA((count,)),
            pltpu.SemaphoreType.DMA,
        ],
        compiler_params=pltpu.CompilerParams(collective_id=number, has_side_effects=True),
        name=f"exchange_{number}",
    )(value)


def across(left, right):
    return lax.dot_general(
        left, right, (((1,), (1,)), ((), ())), preferred_element_type=jnp.float32
    )


def prepare(values, shift, maps, scale, drive_real, drive_imaginary):
    groups, width = shift.shape[1], scale.shape[1]
    spread = lax.broadcasted_iota(jnp.int32, (groups, width), 1) // (width // groups)
    hot = (spread == lax.broadcasted_iota(jnp.int32, (groups, width), 0)).astype(jnp.float32)
    scale[...] = jnp.dot(
        jnp.exp(shift[...]), hot, precision=TOP_PRECISION, preferred_element_type=jnp.float32
    )
    entries = values[...]
    drive_real[...] = across(entries, maps[0]) + across(entries, maps[1])
    drive_imaginary[...] = across(entries, maps[2]) + across(entries, maps[3])


def totals_kernel(values, shift, factor, maps, parts, total, scale, drive_real, drive_imaginary):
    prepare(values, shift, maps, scale, drive_real, drive_imaginary)
    width = scale.shape[1]
    wide = (LANES, width)
    factor_real = jnp.broadcast_to(factor[0:1, :], wide)
    factor_imaginary = jnp.broadcast_to(factor[1:2, :], wide)

    def step(position, carry):
        a_real, a_imaginary, x_real, x_imaginary = carry
        rows = pl.ds(pl.multiple_of(position * LANES, LANES), LANES)
        grow = scale[rows, :]
        b_real, b_imaginary = grow * factor_real, grow * factor_imaginary
        return (
            b_real * a_real - b_imaginary * a_imaginary,
            b_real * a_imaginary + b_imaginary * a_real,
            b_real * x_real - b_imaginary * x_imaginary + drive_real[rows, :],
            b_real * x_imaginary + b_imaginary * x_real + drive_imaginary[rows, :],
        )

    empty = jnp.zeros(wide, jnp.float32)
    ends = lax.fori_loop(
        0, scale.shape[0] // LANES, step, (jnp.ones(wide, jnp.float32), empty, empty, empty)
    )
    for place, end in enumerate(ends):
        parts[place] = end
    run = tuple(end[0:1] for end in ends)
    for segment in range(1, LANES):
        b_real, b_imaginary, y_real, y_imaginary = (
            end[segment : segment + 1] for end in ends
        )
        a_real, a_imaginary, x_real, x_imaginary = run
        run = (
            b_real * a_real - b_imaginary * a_imaginary,
            b_real * a_imaginary + b_imaginary * a_real,
            b_real * x_real - b_imaginary * x_imaginary + y_real,
            b_real * x_imaginary + b_imaginary * x_real + y_imaginary,
        )
    total[...] = jnp.concatenate(run + (jnp.zeros((LANES - 4, width), jnp.float32),), axis=0)


def split(value):
    high = value.astype(jnp.bfloat16)
    return high, (value - high.astype(jnp.float32)).astype(jnp.bfloat16)


def respond_kernel(
    axis, values, shift, factor, maps, parts, gathered, reads, skip, out,
    scale, drive_real, drive_imaginary,
):
    prepare(values, shift, maps, scale, drive_real, drive_imaginary)
    width = scale.shape[1]
    mine = lax.axis_index(axis)

    def before(position, carry):
        real, imaginary = carry
        item = gathered[position]
        a_real, a_imaginary = item[0:1], item[1:2]
        keep = position < mine
        return (
            jnp.where(keep, a_real * real - a_imaginary * imaginary + item[2:3], real),
            jnp.where(keep, a_real * imaginary + a_imaginary * real + item[3:4], imaginary),
        )

    none = jnp.zeros((1, width), jnp.float32)
    real, imaginary = lax.fori_loop(0, gathered.shape[0] - 1, before, (none, none))
    reals, imaginaries = [real], [imaginary]
    for segment in range(LANES - 1):
        at = slice(segment, segment + 1)
        a_real, a_imaginary = parts[0, at, :], parts[1, at, :]
        real, imaginary = (
            a_real * real - a_imaginary * imaginary + parts[2, at, :],
            a_real * imaginary + a_imaginary * real + parts[3, at, :],
        )
        reals.append(real)
        imaginaries.append(imaginary)
    wide = (LANES, width)
    factor_real = jnp.broadcast_to(factor[0:1, :], wide)
    factor_imaginary = jnp.broadcast_to(factor[1:2, :], wide)

    def step(position, carry):
        x_real, x_imaginary = carry
        rows = pl.ds(pl.multiple_of(position * LANES, LANES), LANES)
        grow = scale[rows, :]
        b_real, b_imaginary = grow * factor_real, grow * factor_imaginary
        new_real = b_real * x_real - b_imaginary * x_imaginary + drive_real[rows, :]
        new_imaginary = b_real * x_imaginary + b_imaginary * x_real + drive_imaginary[rows, :]
        drive_real[rows, :] = new_real
        drive_imaginary[rows, :] = new_imaginary
        return new_real, new_imaginary

    lax.fori_loop(
        0,
        scale.shape[0] // LANES,
        step,
        (jnp.concatenate(reals, axis=0), jnp.concatenate(imaginaries, axis=0)),
    )
    high, low = split(drive_real[...])
    response = across(high, reads[0]) + across(low, reads[0]) + across(high, reads[1])
    high, low = split(drive_imaginary[...])
    response -= across(high, reads[2]) + across(low, reads[2]) + across(high, reads[3])
    response += skip[...] * values[...].astype(jnp.float32)
    out[...] = jax.nn.gelu(response).astype(jnp.bfloat16)


def diagonal(blocks):
    groups, rows, columns = blocks.shape
    tiled = jnp.tile(blocks.reshape(groups * rows, columns), (1, groups))
    row = lax.broadcasted_iota(jnp.int32, tiled.shape, 0) // rows
    column = lax.broadcasted_iota(jnp.int32, tiled.shape, 1) // columns
    return split(jnp.where(row == column, tiled, 0.0))


def mixer(mixer_input, decay_shift, factors, readout_matrix, skip):
    factor_real, factor_imaginary, map_real, map_imaginary = factors
    rows, channels = mixer_input.shape
    groups, states = factor_real.shape
    width = groups * states

    def arrange(value):
        return jnp.swapaxes(value.reshape(LANES, rows // LANES, -1), 0, 1).reshape(rows, -1)

    values, shift = arrange(mixer_input), arrange(decay_shift)
    factor = jnp.stack([factor_real.reshape(width), factor_imaginary.reshape(width)])
    maps = jnp.stack(diagonal(map_real) + diagonal(map_imaginary))
    reads = jnp.stack(
        diagonal(readout_matrix[0]) + diagonal(readout_matrix[1])
    )
    vmem = pl.BlockSpec(memory_space=pltpu.VMEM)
    scratch = [pltpu.VMEM((rows, width), jnp.float32)] * 3
    parts, total = pl.pallas_call(
        totals_kernel,
        out_shape=(
            jax.ShapeDtypeStruct((4, LANES, width), jnp.float32),
            jax.ShapeDtypeStruct((LANES, width), jnp.float32),
        ),
        in_specs=[vmem] * 4,
        out_specs=(vmem, vmem),
        scratch_shapes=scratch,
        name="totals",
    )(values, shift, factor, maps)
    gathered = exchange(total, "sp", 0, gather=True)
    activated = pl.pallas_call(
        functools.partial(respond_kernel, "sp"),
        out_shape=jax.ShapeDtypeStruct((rows, channels), jnp.bfloat16),
        in_specs=[vmem] * 8,
        out_specs=vmem,
        scratch_shapes=scratch,
        name="respond",
    )(values, shift, factor, maps, parts, gathered, reads, skip.reshape(1, -1))
    return jnp.swapaxes(activated.reshape(rows // LANES, LANES, channels), 0, 1)


def slot_numbers(route_rows, experts, capacity):
    flat = route_rows.reshape(route_rows.shape[:-2] + (-1,))
    matches = (flat[..., None] == jnp.arange(experts, dtype=jnp.int32)).astype(jnp.int32)
    earlier = jnp.cumsum(matches, axis=-2) - matches
    return flat * capacity + jnp.sum(earlier * matches, axis=-1)


def dispatch_rows(slots, normed, width):
    hits = (slots[..., None] == jnp.arange(width, dtype=jnp.int32)).astype(jnp.bfloat16)
    tokens = normed.shape[-2]
    hits = hits.reshape(slots.shape[:-1] + (tokens, -1, width)).sum(axis=-2)
    return jnp.einsum(
        "...tw,...td->...wd", hits, normed, preferred_element_type=jnp.float32
    ).astype(jnp.bfloat16)


def shards(
    mixer_input,
    decay_shift,
    pole_real,
    pole_imaginary,
    log_step,
    input_map,
    readout_matrix,
    skip,
    out_proj,
    stream,
    norm_gain,
    routes,
    route_logits,
    w_gate,
    w_up,
    w_down,
):
    factors = discretize(pole_real, pole_imaginary, log_step, input_map)
    shares = lax.axis_size("tp")
    own_rows = stream.shape[0]
    activated = mixer(mixer_input, decay_shift, factors, readout_matrix, skip)
    whole_proj = lax.all_gather(out_proj, "tp", axis=0, tiled=True)
    received = exchange(activated.reshape(shares, own_rows, -1), "tp", 1)
    own_activated = jnp.swapaxes(received, 0, 1).reshape(own_rows, -1)
    projected = jnp.dot(own_activated, whole_proj, preferred_element_type=jnp.float32)
    mixed = (stream.astype(jnp.float32) + projected).astype(jnp.bfloat16)
    mixed_wide = mixed.astype(jnp.float32)
    normed = (
        mixed_wide
        * lax.rsqrt(jnp.mean(mixed_wide * mixed_wide, axis=-1, keepdims=True) + EPS)
        * norm_gain
    ).astype(jnp.bfloat16)
    weights = jax.nn.sigmoid(
        jnp.stack(
            [route_logits[:, 0] - route_logits[:, 1], route_logits[:, 1] - route_logits[:, 0]],
            axis=1,
        )
    )
    experts = lax.axis_size("sp") * w_gate.shape[0]
    capacity = 4 * own_rows // experts
    slot_width = experts * capacity
    model = stream.shape[1]
    own_slots = slot_numbers(routes, experts, capacity)
    outgoing = dispatch_rows(own_slots, normed, slot_width)
    arrived = exchange(outgoing.reshape(experts, capacity, model), "sp", 2)
    expert_rows = lax.all_gather(arrived.reshape(-1, model), "tp", axis=0, tiled=True)
    gate = jnp.dot(expert_rows, w_gate[0], preferred_element_type=jnp.float32)
    upward = jnp.dot(expert_rows, w_up[0], preferred_element_type=jnp.float32)
    hidden = (jax.nn.silu(gate) * upward).astype(jnp.bfloat16)
    summed = lax.psum_scatter(
        jnp.dot(hidden, w_down[0], preferred_element_type=jnp.float32).astype(jnp.bfloat16),
        "tp",
        scatter_dimension=0,
        tiled=True,
    )
    expert_out = summed.reshape(-1, capacity, model)
    returned_result = exchange(expert_out, "sp", 3).reshape(slot_width, model)
    picked = (
        jnp.take(returned_result, own_slots, axis=0)
        .astype(jnp.float32)
        .reshape(own_rows, -1, model)
    )
    combined = mixed_wide + jnp.sum(picked * weights[:, :, None], axis=1)
    return combined.astype(jnp.bfloat16)


def solution(mesh):
    return jax.shard_map(
        shards,
        mesh=mesh,
        in_specs=(
            P("sp", "tp"),
            P("sp", "tp"),
            P("tp", None),
            P("tp", None),
            P("tp"),
            P(None, "tp", None, None),
            P(None, "tp", None, None),
            P("tp"),
            P("tp", None),
            P(("sp", "tp"), None),
            P(),
            P(("sp", "tp"), None),
            P(("sp", "tp"), None),
            P("sp", None, "tp"),
            P("sp", None, "tp"),
            P("sp", "tp", None),
        ),
        out_specs=P(("sp", "tp"), None),
        check_vma=False,
    )
```
